32 devices in a mesh: ep: 8 (over z, core), tp: 4 (over y, x).
Axes of the slice: x: 2, y: 2, z: 4, core: 2. Of those that a mesh axis runs over, the one named last changes fastest.
Arguments:
- compressed_query: bfloat16 [1024, 1536], P('ep'), may hold values from -6 to 6
- compressed_key_value: bfloat16 [1024, 512], P('ep'), may hold values from -6 to 6
- rotary_key: bfloat16 [1024, 32], P('ep'), may hold values from -600 to 600
- query_norm_scale: float32 [1536], replicated, may hold values from 0.1 to 1.9
- context_norm_scale: float32 [512], replicated, may hold values from 0.1 to 1.9
- query_plain_weight: bfloat16 [1536, 1024], P(None, 'tp'), may hold values from -0.375 to 0.375
- query_rotary_weight: bfloat16 [1536, 512], P(None, 'tp'), may hold values from -0.375 to 0.375
- key_up_weight: bfloat16 [512, 1024], P(None, 'tp'), may hold values from -0.25 to 0.25
- value_up_weight: bfloat16 [512, 1024], P(None, 'tp'), may hold values from -0.25 to 0.25
- output_weight: bfloat16 [1024, 2048], P(None, 'tp'), may hold values from -0.75 to 0.75
- mixture_input: bfloat16 [1024, 2048], P('ep'), may hold values from -6 to 6
- mixture_gain: float32 [2048], replicated, may hold values from 0.1 to 1.9
- routes: int32 [1024, 2], P('ep'), may hold values from 0 to 7, all different within a row; in each aligned block of 128 rows (0 to 127, 128 to 255, ...) at most 48 rows name the same one
- route_weight: float32 [1024, 2], P('ep'), may hold values from 0.2 to 2
- expert_gate: bfloat16 [8, 2048, 4096], P('ep', None, 'tp'), may hold values from -0.125 to 0.125
- expert_up: bfloat16 [8, 2048, 4096], P('ep', None, 'tp'), may hold values from -0.125 to 0.125
- expert_down: bfloat16 [8, 4096, 2048], P('ep', None, 'tp'), may hold values from -0.09375 to 0.09375
- shared_gate: bfloat16 [2048, 512], P(None, 'tp'), may hold values from -0.125 to 0.125
- shared_up: bfloat16 [2048, 512], P(None, 'tp'), may hold values from -0.125 to 0.125
- shared_down: bfloat16 [512, 2048], P(None, 'tp'), may hold values from -0.25 to 0.25
Outputs:
- attended: bfloat16 [1024, 2048], P('ep', 'tp')
- combined: bfloat16 [1024, 2048], P('ep', 'tp')
The draws below stay inside these ranges and needn't reach their ends.
Inputs may be any that keep to these rules, and one draw needn't show every extreme that they name: `routes`: in the rows of each index of ep, no expert is named more than 48 times, a bound that some block reaches there.
All inputs are finite; a program needn't handle non-finite values.
Results may differ from the reference program's by a relative error of at most 0.012.
The reference program's roundings to bfloat16 on the way count: a program that leaves them out, or rounds other values in their place, can miss the bound.
Values may be sent and summed in bfloat16 or wider, within the bound.
No kernel may reach another device: no remote copies, remote signals or barrier semaphores. Data moves between devices by JAX's collectives and lax.ppermute only.
A program may use at most 64 MiB of HBM per device.

```python
import math
import jax
import jax.numpy as jnp
import numpy as np
from jax import lax

D = 2048
HEAD_COUNT = 16
PLAIN_HEAD_SIZE = 64
ROTARY_SIZE = 32
VALUE_HEAD_SIZE = 64
QUERY_RANK = 1536
KEY_VALUE_RANK = 512
EXP_FF = 4096
SH_FF = 512
TOPK = 2
TOK2 = 128
SEQUENCE_LEN1 = 1024
TOKENS2 = 1024
EXPERTS = 8
CAP = 48
N_EP = 8


def draw_rotary_key(key, part):
    base = jax.random.normal(key, (SEQUENCE_LEN1, ROTARY_SIZE), jnp.float32)
    return base.astype(jnp.bfloat16)


def levels(rng, extent, pieces, least, high):
    loudness, own = 1.0, jax.random.fold_in(rng, 6)
    for dim, parts in pieces:
        heights = jnp.exp(jax.random.uniform(jax.random.fold_in(own, dim), (parts,), jnp.float32, least / len(pieces), high / len(pieces)))
        loudness = loudness * jnp.repeat(heights, extent[dim] // parts).reshape([-1 if axis == dim else 1 for axis in range(len(extent))])
    return loudness


def assign_block(rng, own, number, rows, number_of, top, most, lean):
    order = jax.random.permutation(rng, number_of)
    packed, common = load_shares(number_of, rows * top, most, lean, True), load_shares(number_of, rows * top, most, lean, False)
    places = jnp.arange(number_of)

    def named(tallies, offset_by):
        used = int((tallies > 0).sum())
        fixed = max(1, used // 4)
        moved = fixed + (places - fixed + offset_by * (used - fixed)) % max(1, number_of - fixed)
        return jnp.zeros((number_of,), jnp.int32).at[order[jnp.where(places < fixed, places, moved)]].set(jnp.asarray(tallies, jnp.int32))

    tallies = jnp.where(number % 4 == 0, named(packed, number // 4), named(common, number - number // 4 - 1))
    mixed = jax.random.permutation(jax.random.fold_in(own, 3), number_of)
    donor, sink = mixed[0:number_of // 2 * 2:2], mixed[1:number_of // 2 * 2:2]
    room = jnp.minimum(tallies[donor] - 1, most - tallies[sink]) // 2
    room = jnp.where((donor == order[0]) | (sink == order[0]) | (tallies[sink] == 0), 0, jnp.maximum(room, 0))
    moved = jax.random.randint(jax.random.fold_in(own, 4), (number_of // 2,), 0, 1 << 20) % (room + 1)
    tallies = tallies.at[donor].add(-moved).at[sink].add(moved)
    members = jnp.searchsorted(jnp.cumsum(tallies), jnp.arange(rows * top), side="right").astype(jnp.int32)
    listing = members.reshape(top, rows).T
    listing = listing[jax.random.permutation(jax.random.fold_in(own, 1), rows)]
    offset_by = jax.random.randint(jax.random.fold_in(own, 2), (rows, 1), 0, top)
    return jnp.take_along_axis(listing, (jnp.arange(top)[None, :] + offset_by) % top, axis=1)


def load_shares(count, total, limit, slope, full):
    loads = [(1 << 20) // math.isqrt(grade ** slope) + 1 for grade in range(1, count + 1)]
    largest = limit if full else min(limit, max(-(-total // count), total * loads[0] // sum(loads)))
    least = 1 if total - largest >= count - 1 else 0
    given, surplus = [largest] + [least] * (count - 1), total - largest - least * (count - 1)
    while surplus > 0:
        candidates = [i for i in range(1, count) if given[i] < largest] or [i for i in range(1, count) if given[i] < limit]
        pool, remaining = sum([loads[i] for i in candidates]), surplus
        for i in candidates:
            addition = min(limit - given[i], max(1, remaining * loads[i] // pool), surplus)
            given[i] = given[i] + addition
            surplus = surplus - addition
    return np.array(given)


def noise(own_key, extent, deviation, bound, cuts=(), kind=jnp.bfloat16):
    factor_of = levels(own_key, extent, cuts, -0.22, 0.18) if cuts else 1.0
    result = jax.random.normal(own_key, extent, jnp.float32) * deviation * factor_of
    return jnp.minimum(jnp.maximum(result, -bound), bound).astype(kind)


def setup_inputs(seed: int = 0) -> dict:
    arg_keys = jax.random.split(jax.random.key(seed), 21)
    compressed_query = noise(arg_keys[0], (SEQUENCE_LEN1, QUERY_RANK), 1.0, 6.0, ((0, 8),))
    compressed_key_value = noise(arg_keys[1], (SEQUENCE_LEN1, KEY_VALUE_RANK), 1.0, 6.0, ((0, 8),))
    rotary_key = draw_rotary_key(jax.random.fold_in(arg_keys[20], 71), 0)
    query_norm_scale = jnp.clip(1.0 + 0.18 * jax.random.normal(arg_keys[3], (QUERY_RANK,), jnp.float32), 0.1, 1.9)
    context_norm_scale = jnp.clip(1.0 + 0.18 * jax.random.normal(arg_keys[4], (KEY_VALUE_RANK,), jnp.float32), 0.1, 1.9)
    query_plain_weight = noise(arg_keys[5], (QUERY_RANK, HEAD_COUNT * PLAIN_HEAD_SIZE), (QUERY_RANK // 6) ** -0.5, 0.375, ((1, 4),))
    query_rotary_weight = noise(arg_keys[6], (QUERY_RANK, HEAD_COUNT * ROTARY_SIZE), (QUERY_RANK // 6) ** -0.5, 0.375, ((1, 4),))
    key_up_weight = noise(arg_keys[7], (KEY_VALUE_RANK, HEAD_COUNT * PLAIN_HEAD_SIZE), KEY_VALUE_RANK ** -0.5, 0.25, ((1, 4),))
    value_up_weight = noise(arg_keys[8], (KEY_VALUE_RANK, HEAD_COUNT * VALUE_HEAD_SIZE), KEY_VALUE_RANK ** -0.5, 0.25, ((1, 4),))
    output_weight = noise(arg_keys[9], (HEAD_COUNT * VALUE_HEAD_SIZE, D), (HEAD_COUNT * VALUE_HEAD_SIZE // 16) ** -0.5, 0.75, ((1, 4),))
    mixture_input = noise(arg_keys[10], (TOKENS2, D), 1.0, 6.0, ((0, 8),))
    mixture_gain = jnp.clip(1.0 + 0.18 * jax.random.normal(arg_keys[11], (D,), jnp.float32), 0.1, 1.9)
    routes_keys = jax.random.split(jax.random.fold_in(arg_keys[12], 1), TOKENS2 // TOK2)
    routes_turns = jax.random.permutation(jax.random.fold_in(arg_keys[12], 3), TOKENS2 // TOK2)
    routes = jax.vmap(lambda own, number: assign_block(jax.random.fold_in(arg_keys[12], 2), own, number, TOK2, EXPERTS, TOPK, CAP, 1))(routes_keys, routes_turns).reshape((TOKENS2, TOPK))
    route_weight = jnp.clip(0.2 + 1.8 * jax.random.uniform(arg_keys[13], (TOKENS2, TOPK), jnp.float32) ** levels(arg_keys[13], (TOKENS2, TOPK), ((0, 8),), -0.2, 0.2), 0.2, 2.0)
    expert_gate = noise(arg_keys[14], (EXPERTS, D, EXP_FF), D ** -0.5, 0.125, ((0, 8), (2, 4)))
    expert_up = noise(arg_keys[15], (EXPERTS, D, EXP_FF), D ** -0.5, 0.125, ((0, 8), (2, 4)))
    expert_down = noise(arg_keys[16], (EXPERTS, EXP_FF, D), EXP_FF ** -0.5, 0.09375, ((0, 8), (2, 4)))
    shared_gate = noise(arg_keys[17], (D, SH_FF), D ** -0.5, 0.125, ((1, 4),))
    shared_up = noise(arg_keys[18], (D, SH_FF), D ** -0.5, 0.125, ((1, 4),))
    shared_down = noise(arg_keys[19], (SH_FF, D), SH_FF ** -0.5, 0.25, ((1, 4),))
    return dict(compressed_query=compressed_query, compressed_key_value=compressed_key_value, rotary_key=rotary_key, query_norm_scale=query_norm_scale, context_norm_scale=context_norm_scale, query_plain_weight=query_plain_weight, query_rotary_weight=query_rotary_weight, key_up_weight=key_up_weight, value_up_weight=value_up_weight, output_weight=output_weight, mixture_input=mixture_input, mixture_gain=mixture_gain, routes=routes, route_weight=route_weight, expert_gate=expert_gate, expert_up=expert_up, expert_down=expert_down, shared_gate=shared_gate, shared_up=shared_up, shared_down=shared_down)


def normed_rows(values, scaling):
    floats = values.astype(jnp.float32)
    return floats * lax.rsqrt(lax.optimization_barrier(jnp.mean(floats * floats, axis=-1, keepdims=True)) + 1e-06) * scaling

def rotary_tables(positions):
    inverse = 1.0 / 10000.0 ** (jnp.arange(0, ROTARY_SIZE, 2, dtype=jnp.float32) / ROTARY_SIZE)
    angles = positions.astype(jnp.float32)[:, None] * inverse[None, :]
    return (jnp.cos(angles), jnp.sin(angles))

def rotate(vectors, cosine, sine_part):
    half_width = vectors.shape[-1] // 2
    front_half = vectors[..., :half_width]
    back_half = vectors[..., half_width:]
    return jnp.concatenate([front_half * cosine - back_half * sine_part, front_half * sine_part + back_half * cosine], axis=-1)

def reference(compressed_query, compressed_key_value, rotary_key, query_norm_scale, context_norm_scale, query_plain_weight, query_rotary_weight, key_up_weight, value_up_weight, output_weight, mixture_input, mixture_gain, routes, route_weight, expert_gate, expert_up, expert_down, shared_gate, shared_up, shared_down):
    positions = jnp.arange(SEQUENCE_LEN1, dtype=jnp.int32)
    cosine, sine_part = rotary_tables(positions)
    compressed = normed_rows(compressed_query, query_norm_scale).astype(jnp.bfloat16)
    query_nope = jnp.dot(compressed, query_plain_weight, preferred_element_type=jnp.float32).astype(jnp.bfloat16)
    query_turn = jnp.dot(compressed, query_rotary_weight, preferred_element_type=jnp.float32).reshape(SEQUENCE_LEN1, HEAD_COUNT, ROTARY_SIZE)
    query_rot = rotate(query_turn, cosine[:, None, :], sine_part[:, None, :])
    context = normed_rows(compressed_key_value, context_norm_scale).astype(jnp.bfloat16)
    key_rot = rotate(rotary_key.astype(jnp.float32), cosine, sine_part)
    key_nope = jnp.dot(context, key_up_weight, preferred_element_type=jnp.float32).astype(jnp.bfloat16)
    value_rows = jnp.dot(context, value_up_weight, preferred_element_type=jnp.float32).astype(jnp.bfloat16)
    scale = (PLAIN_HEAD_SIZE + ROTARY_SIZE) ** (-0.5)
    rows_block = math.gcd(SEQUENCE_LEN1, 512)

    def per_head(inputs):
        head_query, head_turn, head_key, head_value = inputs

        def per_block(block_inputs):
            block_query, block_turn = block_inputs
            scores = (jnp.dot(block_query, head_key.T, preferred_element_type=jnp.float32) + jnp.dot(block_turn, key_rot.T, precision=lax.Precision.HIGHEST)) * scale
            largest = lax.optimization_barrier(jnp.max(scores, axis=-1, keepdims=True))
            weights = jnp.exp(scores - largest)
            summed = jnp.dot(weights.astype(jnp.bfloat16), head_value, preferred_element_type=jnp.float32)
            return (summed / lax.optimization_barrier(jnp.sum(weights, axis=-1, keepdims=True))).astype(jnp.bfloat16)
        blocks = lax.map(per_block, (head_query.reshape(SEQUENCE_LEN1 // rows_block, rows_block, PLAIN_HEAD_SIZE), head_turn.reshape(SEQUENCE_LEN1 // rows_block, rows_block, ROTARY_SIZE)))
        return blocks.reshape(SEQUENCE_LEN1, VALUE_HEAD_SIZE)
    heads_out = lax.map(per_head, (query_nope.reshape(SEQUENCE_LEN1, HEAD_COUNT, PLAIN_HEAD_SIZE).transpose(1, 0, 2), query_rot.transpose(1, 0, 2), key_nope.reshape(SEQUENCE_LEN1, HEAD_COUNT, PLAIN_HEAD_SIZE).transpose(1, 0, 2), value_rows.reshape(SEQUENCE_LEN1, HEAD_COUNT, VALUE_HEAD_SIZE).transpose(1, 0, 2)))
    heads_out = heads_out.transpose(1, 0, 2).reshape(SEQUENCE_LEN1, HEAD_COUNT * VALUE_HEAD_SIZE)
    attended = jnp.dot(heads_out, output_weight, preferred_element_type=jnp.float32).astype(jnp.bfloat16)
    floats = mixture_input.astype(jnp.float32)
    centred = floats - lax.optimization_barrier(jnp.mean(floats, axis=-1, keepdims=True))
    normed = (centred * lax.rsqrt(lax.optimization_barrier(jnp.mean(centred * centred, axis=-1, keepdims=True)) + 1e-05) * mixture_gain).astype(jnp.bfloat16)
    shared_hidden = (jax.nn.silu(jnp.dot(normed, shared_gate, preferred_element_type=jnp.float32)) * jnp.dot(normed, shared_up, preferred_element_type=jnp.float32)).astype(jnp.bfloat16)
    flat_routes = routes.reshape(N_EP, TOK2 * TOPK)
    one_hot = (flat_routes[:, :, None] == jnp.arange(EXPERTS, dtype=jnp.int32)[None, None, :]).astype(jnp.int32)
    ranks = lax.optimization_barrier(jnp.sum(one_hot * (jnp.cumsum(one_hot, axis=1) - 1), axis=-1))
    sources = jnp.arange(N_EP, dtype=jnp.int32)[:, None]
    place = flat_routes * (N_EP * CAP) + sources * CAP + ranks
    token_ids = sources * TOK2 + jnp.arange(TOK2 * TOPK, dtype=jnp.int32)[None, :] // TOPK
    owners = jnp.full((EXPERTS * N_EP * CAP,), TOKENS2, jnp.int32)
    owners = owners.at[place.reshape(-1)].set(token_ids.reshape(-1)).reshape(EXPERTS, N_EP * CAP)
    padded = jnp.concatenate([normed, jnp.zeros((1, D), jnp.bfloat16)], axis=0)

    def per_expert(inputs):
        owner_rows, gate_matrix, up_matrix, down_matrix = inputs
        gathered = padded[owner_rows]
        hidden = (jax.nn.silu(jnp.dot(gathered, gate_matrix, preferred_element_type=jnp.float32)) * jnp.dot(gathered, up_matrix, preferred_element_type=jnp.float32)).astype(jnp.bfloat16)
        return jnp.dot(hidden, down_matrix, preferred_element_type=jnp.float32).astype(jnp.bfloat16)
    results = lax.map(per_expert, (owners, expert_gate, expert_up, expert_down))
    picked = results.reshape(EXPERTS * N_EP * CAP, D)[place.reshape(-1)]
    picked = picked.astype(jnp.float32).reshape(TOKENS2, TOPK, D)
    routed = lax.optimization_barrier(jnp.sum(picked * route_weight[:, :, None], axis=1))
    combined = (jnp.dot(shared_hidden, shared_down, preferred_element_type=jnp.float32) + routed).astype(jnp.bfloat16)
    return (attended, combined)
```

```python
import functools

import jax
import jax.numpy as jnp
from jax import lax
from jax.experimental import pallas as pl
from jax.experimental.pallas import tpu as pltpu
from jax.sharding import PartitionSpec as P

PLAIN_HEAD_SIZE = 64
ROTARY_SIZE = 32
VALUE_HEAD_SIZE = 64
TOPK = 2
BF16 = jnp.bfloat16
F32 = jnp.float32


def dot(a, b):
    return jnp.dot(a, b, preferred_element_type=F32)


def dot_rows(a, b):
    return lax.dot_general(a, b, (((1,), (1,)), ((), ())), preferred_element_type=F32)


def centred_rows(x):
    x = x.astype(F32)
    mean = jnp.mean(x, axis=-1, keepdims=True)
    centred = x - mean
    return mean, lax.rsqrt(jnp.mean(centred * centred, axis=-1, keepdims=True) + 1e-05)


def slot_columns(routes, base, experts, capacity):
    tokens = routes.shape[0]
    lanes = lax.broadcasted_iota(jnp.int32, (tokens, experts), 1)
    marks = [(lanes == routes[:, k : k + 1]).astype(F32) for k in range(TOPK)]
    row = lax.broadcasted_iota(jnp.int32, (tokens, tokens), 0)
    col = lax.broadcasted_iota(jnp.int32, (tokens, tokens), 1)
    earlier = (col < row).astype(BF16)
    before = dot(earlier, sum(marks).astype(BF16))
    first = ((lanes ^ base) * capacity).astype(F32) + before
    return [jnp.sum(m * first, axis=1, keepdims=True).astype(jnp.int32) for m in marks]


def picked(slot, count):
    lanes = lax.broadcasted_iota(jnp.int32, (slot.shape[0], count), 1)
    return (lanes == slot).astype(BF16)


def dispatch_kernel(place, routes_ref, x_ref, part_ref, gain_ref, *outs, experts, capacity):
    mean, scale = centred_rows(x_ref[...])
    normed = ((part_ref[...].astype(F32) - mean) * scale * gain_ref[...]).astype(BF16)
    count = experts * capacity
    slots = slot_columns(routes_ref[...], place[0], experts, capacity)
    chosen = picked(slots[0], count) + picked(slots[1], count)
    rows = lax.dot_general(
        chosen, normed, (((0,), (0,)), ((), ())), preferred_element_type=F32
    ).astype(BF16)
    each = count // len(outs)
    for k, out in enumerate(outs):
        out[...] = rows[k * each : (k + 1) * each]


def dispatch(place, routes, x, gain, experts, capacity, width, pieces):
    tokens, model = x.shape
    each = experts * capacity // pieces
    return pl.pallas_call(
        functools.partial(dispatch_kernel, experts=experts, capacity=capacity),
        grid_spec=pltpu.PrefetchScalarGridSpec(
            num_scalar_prefetch=1,
            grid=(1,),
            in_specs=[
                pl.BlockSpec((tokens, TOPK), lambda i, s: (0, 0)),
                pl.BlockSpec((tokens, model), lambda i, s: (0, 0)),
                pl.BlockSpec((tokens, width), lambda i, s: (0, s[1])),
                pl.BlockSpec((1, width), lambda i, s: (0, s[1])),
            ],
            out_specs=[pl.BlockSpec((each, width), lambda i, s: (0, 0))] * pieces,
        ),
        out_shape=[jax.ShapeDtypeStruct((each, width), BF16)] * pieces,
        name="dispatch",
    )(place, routes, x, x, gain)


def shared_kernel(x_ref, gain_ref, gate_ref, up_ref, out):
    mean, scale = centred_rows(x_ref[...])
    normed = ((x_ref[...].astype(F32) - mean) * scale * gain_ref[...]).astype(BF16)
    gate = dot(normed, gate_ref[...])
    out[...] = (gate / (1.0 + jnp.exp(-gate)) * dot(normed, up_ref[...])).astype(BF16)


def thirds(x):
    one = x.astype(BF16)
    rest = x - one.astype(F32)
    two = rest.astype(BF16)
    return one, two, (rest - two.astype(F32)).astype(BF16)


def turned(vectors, cosine, sine):
    half = vectors.shape[1] // 2
    a, b = vectors[:, :half], vectors[:, half:]
    return jnp.concatenate([a * cosine - b * sine, a * sine + b * cosine], axis=1)


def rms_rows(x, scale):
    x = x.astype(F32)
    return (x * lax.rsqrt(jnp.mean(x * x, axis=-1, keepdims=True) + 1e-06) * scale).astype(BF16)


def latent_kernel(kv_ref, scale_ref, key_ref, cos_ref, sin_ref, out):
    rank = kv_ref.shape[1]
    out[:, :rank] = rms_rows(kv_ref[...], scale_ref[...])
    parts = thirds(turned(key_ref[...].astype(F32), cos_ref[...], sin_ref[...]))
    spare = jnp.zeros((kv_ref.shape[0], out.shape[1] - rank - 3 * ROTARY_SIZE), BF16)
    out[:, rank:] = jnp.concatenate([*parts, spare], axis=1)


def query_kernel(q_ref, scale_ref, plain_ref, rotary_ref, cos_ref, sin_ref, plain_out, turn_out):
    compressed = rms_rows(q_ref[...], scale_ref[...])
    plain_out[...] = dot(compressed, plain_ref[...]).astype(BF16)
    turns = dot(compressed, rotary_ref[...])
    for h in range(turn_out.shape[0]):
        turn = turns[:, h * ROTARY_SIZE : (h + 1) * ROTARY_SIZE]
        one, two, three = thirds(turned(turn, cos_ref[...], sin_ref[...]))
        turn_out[h] = jnp.concatenate([one, one, two, two, one, three], axis=1)


def attend_kernel(plain_ref, turn_ref, shared_ref, key_ref, value_ref, *rest, heads, rank):
    *blocks, out, keys, values, turns = rest
    at = 0
    for block in blocks:
        rows = block.shape[0]
        latent = block[:, :rank]
        keys[at : at + rows] = dot(latent, key_ref[...]).astype(BF16)
        values[at : at + rows] = dot(latent, value_ref[...]).astype(BF16)
        rot = block[:, rank:]
        one, two, three = (rot[:, i * ROTARY_SIZE : (i + 1) * ROTARY_SIZE] for i in range(3))
        turns[at : at + rows] = jnp.concatenate([one, two, one, two, three, one], axis=1)
        at += rows
    scale = (PLAIN_HEAD_SIZE + ROTARY_SIZE) ** (-0.5)
    plain = plain_ref[...]
    lanes = lax.broadcasted_iota(jnp.int32, plain.shape, 1) // PLAIN_HEAD_SIZE
    total = jnp.zeros(plain.shape, F32)
    for h in range(heads):
        mine = jnp.where(lanes == h, plain, jnp.zeros_like(plain))
        scores = (dot_rows(mine, keys[...]) + dot_rows(turn_ref[h], turns[...])) * scale
        weights = jnp.exp(scores - jnp.max(scores, axis=1, keepdims=True))
        summed = dot(weights.astype(BF16), values[...])
        total = jnp.where(lanes == h, summed / jnp.sum(weights, axis=1, keepdims=True), total)
    width = plain.shape[1]
    out[:, :width] = total.astype(BF16)
    out[:, width:] = shared_ref[...]


def finish_kernel(place, output_ref, down_ref, *rest, heads_width, shared_width, total):
    *pieces, attended_out, shared_out = rest
    views = [p[...] for p in pieces] if len(pieces) > 1 else [pieces[0][j] for j in range(total)]
    attended = shared = 0.0
    for j, view in enumerate(views):
        owner = place[1] ^ j if len(pieces) > 1 else j
        rows = pl.ds(pl.multiple_of(owner * heads_width, heads_width), heads_width)
        attended += dot(view[:, :heads_width], output_ref[rows, :])
        rows = pl.ds(pl.multiple_of(owner * shared_width, shared_width), shared_width)
        shared += dot(view[:, heads_width:], down_ref[rows, :])
    attended_out[...] = attended.astype(BF16)
    shared_out[...] = shared


def hidden_kernel(place, gate_ref, up_ref, *rest):
    *pieces, out = rest
    gate = up = 0.0
    for j, piece in enumerate(pieces):
        width = piece.shape[1]
        owner = place[1] ^ j if len(pieces) > 1 else 0
        rows = pl.ds(pl.multiple_of(owner * width, width), width)
        gate += dot(piece[...], gate_ref[0, rows, :])
        up += dot(piece[...], up_ref[0, rows, :])
    out[...] = (gate / (1.0 + jnp.exp(-gate)) * up).astype(BF16)


def expert_hidden(place, pieces, gate, up):
    rows, width = pieces[0].shape
    _, model, units = gate.shape
    tile = min(units, 256)
    weight = pl.BlockSpec((1, model, tile), lambda i, s: (0, 0, i))
    return pl.pallas_call(
        hidden_kernel,
        grid_spec=pltpu.PrefetchScalarGridSpec(
            num_scalar_prefetch=1,
            grid=(units // tile,),
            in_specs=[weight, weight]
            + [pl.BlockSpec((rows, width), lambda i, s: (0, 0))] * len(pieces),
            out_specs=pl.BlockSpec((rows, tile), lambda i, s: (0, i)),
        ),
        out_shape=jax.ShapeDtypeStruct((rows, units), BF16),
        cost_estimate=pl.CostEstimate(
            flops=4 * rows * model * units, bytes_accessed=4 * model * units, transcendentals=0
        ),
        name="hidden",
    )(place, gate, up, *pieces)


def down_kernel(place, down_ref, *rest, count):
    pieces, outs = rest[:count], rest[count:]
    total = 0.0
    for j, piece in enumerate(pieces):
        width = piece.shape[1]
        owner = place[1] ^ j if count > 1 else 0
        rows = pl.ds(pl.multiple_of(owner * width, width), width)
        total += dot(piece[...], down_ref[0, rows, :])
    result = total.astype(BF16)
    each = result.shape[0] // len(outs)
    for k, out in enumerate(outs):
        out[...] = result[k * each : (k + 1) * each]


def expert_down_rows(place, pieces, down, parts):
    rows, width = pieces[0].shape
    _, units, features = down.shape
    tile = min(features, 256)
    each = rows // parts
    return pl.pallas_call(
        functools.partial(down_kernel, count=len(pieces)),
        grid_spec=pltpu.PrefetchScalarGridSpec(
            num_scalar_prefetch=1,
            grid=(features // tile,),
            in_specs=[pl.BlockSpec((1, units, tile), lambda i, s: (0, 0, i))]
            + [pl.BlockSpec((rows, width), lambda i, s: (0, 0))] * len(pieces),
            out_specs=[pl.BlockSpec((each, tile), lambda i, s: (0, i))] * parts,
        ),
        out_shape=[jax.ShapeDtypeStruct((each, features), BF16)] * parts,
        cost_estimate=pl.CostEstimate(
            flops=2 * rows * units * features,
            bytes_accessed=2 * units * features,
            transcendentals=0,
        ),
        name="down",
    )(place, down, *pieces)


def combine_kernel(place, routes_ref, weight_ref, shared_ref, *rest, experts, capacity):
    *returned, out = rest
    rows = jnp.concatenate([r[...] for r in returned], axis=0)
    slots = slot_columns(routes_ref[...], place[0], experts, capacity)
    routed = 0.0
    for k in range(TOPK):
        routed += dot(picked(slots[k], rows.shape[0]), rows) * weight_ref[:, k : k + 1]
    out[...] = (shared_ref[...] + routed).astype(BF16)


def whole_call(kernel, out_shape, name, *args, scratch=(), place=None, flops=0):
    extra = {}
    if place is not None:
        args = (place, *args)
        extra["in_specs"] = [pl.BlockSpec(memory_space=pltpu.SMEM)] + [
            pl.BlockSpec(memory_space=pltpu.VMEM) for _ in args[1:]
        ]
    if flops:
        extra["cost_estimate"] = pl.CostEstimate(flops=flops, bytes_accessed=0, transcendentals=0)
    return pl.pallas_call(
        kernel, out_shape=out_shape, scratch_shapes=list(scratch), name=name, **extra
    )(*args)


def per_device(
    compressed_query,
    compressed_key_value,
    rotary_key,
    query_norm_scale,
    context_norm_scale,
    query_plain_weight,
    query_rotary_weight,
    key_up_weight,
    value_up_weight,
    output_weight,
    mixture_input,
    mixture_gain,
    routes,
    route_weight,
    expert_gate,
    expert_up,
    expert_down,
    shared_gate,
    shared_up,
    shared_down,
):
    experts, parts = lax.axis_size("ep"), lax.axis_size("tp")
    rank_ep, rank_tp = lax.axis_index("ep"), lax.axis_index("tp")
    direct = experts == 8 and parts == 4
    tokens, model = mixture_input.shape
    capacity = tokens * TOPK * 3 // (2 * experts)
    heads_here = query_plain_weight.shape[1] // PLAIN_HEAD_SIZE
    place = jnp.stack([rank_ep if direct else jnp.zeros_like(rank_ep), rank_tp]).astype(jnp.int32)

    def over_ep(value, k):
        return lax.ppermute(value, "ep", [(i, i ^ k) for i in range(experts)])

    def over_tp(value, k):
        return lax.ppermute(value, "tp", [(i, i ^ k) for i in range(parts)])

    width = model // parts
    gain = mixture_gain.reshape(1, model)
    sent = dispatch(
        place, routes, mixture_input, gain, experts, capacity, width, experts if direct else 1
    )
    if direct:
        chunks = [list(range(0, experts, 2)), list(range(1, experts, 2))]
        arrived = [[over_ep(sent[k], k) if k else sent[k] for k in chunk] for chunk in chunks]
    else:
        chunks = [[0]]
        arrived = [
            [
                lax.all_to_all(
                    sent[0].reshape(experts, capacity, width),
                    "ep",
                    split_axis=0,
                    concat_axis=0,
                    tiled=True,
                ).reshape(experts * capacity, width)
            ]
        ]

    positions = rank_ep * tokens + jnp.arange(compressed_query.shape[0], dtype=jnp.int32)
    inverse = 1.0 / 10000.0 ** (jnp.arange(0, ROTARY_SIZE, 2, dtype=F32) / ROTARY_SIZE)
    angles = positions.astype(F32)[:, None] * inverse[None, :]
    cosine, sine = jnp.cos(angles), jnp.sin(angles)
    rank = compressed_key_value.shape[1]
    latent = whole_call(
        latent_kernel,
        jax.ShapeDtypeStruct((tokens, rank + 128), BF16),
        "latent",
        compressed_key_value,
        context_norm_scale.reshape(1, rank),
        rotary_key,
        cosine,
        sine,
    )
    if direct:
        mine = [over_ep(latent, k) if k else latent for k in range(0, experts, 2)]
        blocks = mine + [over_ep(m, 1) for m in mine]
    else:
        blocks = [lax.all_gather(latent, "ep", axis=0, tiled=True)]
    plain, turns = whole_call(
        query_kernel,
        [
            jax.ShapeDtypeStruct((tokens, query_plain_weight.shape[1]), BF16),
            jax.ShapeDtypeStruct((heads_here, tokens, 6 * ROTARY_SIZE), BF16),
        ],
        "query",
        compressed_query,
        query_norm_scale.reshape(1, -1),
        query_plain_weight,
        query_rotary_weight,
        cosine,
        sine,
    )
    shared_hidden = whole_call(
        shared_kernel,
        jax.ShapeDtypeStruct((tokens, shared_gate.shape[1]), BF16),
        "shared",
        mixture_input,
        gain,
        shared_gate,
        shared_up,
    )

    def gathered(value, chunk):
        if not direct:
            return [lax.all_gather(value, "tp", axis=1, tiled=True)]
        one, two = over_tp(value, 1), over_tp(value, 2)
        return [value, one, two, over_tp(one, 2) if chunk % 2 == 0 else over_tp(two, 1)]

    hidden = []
    for c in range(len(chunks)):
        rows = jnp.concatenate(arrived[c], axis=0) if len(arrived[c]) > 1 else arrived[c][0]
        hidden.append(expert_hidden(place, gathered(rows, c), expert_gate, expert_up))
    returned = [None] * (experts if direct else 1)
    for c, chunk in enumerate(chunks):
        results = expert_down_rows(place, gathered(hidden[c], c), expert_down, len(chunk))
        for k, result in zip(chunk, results):
            if direct:
                returned[k] = over_ep(result, k) if k else result
            else:
                returned[0] = lax.all_to_all(
                    result.reshape(experts, capacity, -1),
                    "ep",
                    split_axis=0,
                    concat_axis=0,
                    tiled=True,
                ).reshape(experts * capacity, -1)

    sequence = tokens * experts
    heads_width, shared_width = query_plain_weight.shape[1], shared_gate.shape[1]
    both = whole_call(
        functools.partial(attend_kernel, heads=heads_here, rank=rank),
        jax.ShapeDtypeStruct((tokens, heads_width + shared_width), BF16),
        "attend",
        plain,
        turns,
        shared_hidden,
        key_up_weight,
        value_up_weight,
        *blocks,
        scratch=[
            pltpu.VMEM((sequence, heads_width), BF16),
            pltpu.VMEM((sequence, heads_width), BF16),
            pltpu.VMEM((sequence, 6 * ROTARY_SIZE), BF16),
        ],
        flops=4 * sequence * rank * heads_width,
    )
    if direct:
        pieces = [over_tp(both, k) if k else both for k in range(parts)]
    else:
        pieces = [lax.all_gather(both, "tp", axis=0)]
    features = output_weight.shape[1]
    attended, shared_part = whole_call(
        functools.partial(
            finish_kernel, heads_width=heads_width, shared_width=shared_width, total=parts
        ),
        [
            jax.ShapeDtypeStruct((tokens, features), BF16),
            jax.ShapeDtypeStruct((tokens, features), F32),
        ],
        "finish",
        output_weight,
        shared_down,
        *pieces,
        place=place,
    )
    combined = whole_call(
        functools.partial(combine_kernel, experts=experts, capacity=capacity),
        jax.ShapeDtypeStruct((tokens, features), BF16),
        "combine",
        routes,
        route_weight,
        shared_part,
        *returned,
        place=place,
    )
    return (attended, combined)


def solution(mesh):
    in_specs = (
        P("ep", None),
        P("ep", None),
        P("ep", None),
        P(),
        P(),
        P(None, "tp"),
        P(None, "tp"),
        P(None, "tp"),
        P(None, "tp"),
        P(None, "tp"),
        P("ep", None),
        P(),
        P("ep", None),
        P("ep", None),
        P("ep", None, "tp"),
        P("ep", None, "tp"),
        P("ep", None, "tp"),
        P(None, "tp"),
        P(None, "tp"),
        P(None, "tp"),
    )
    out_specs = (P("ep", "tp"), P("ep", "tp"))
    return jax.shard_map(
        per_device, mesh=mesh, in_specs=in_specs, out_specs=out_specs, check_vma=False
    )
```
